32 devices in a mesh: tp: 16 (over z, y, x), dp: 2 (over core).
Axes of the slice: x: 2, y: 2, z: 4, core: 2. Of those that a mesh axis runs over, the one named last changes fastest.
Arguments:
- residual_in: bfloat16 [24, 4096], P(None, ('dp', 'tp')), may hold values from -40 to 40
- norm_gain: float32 [2, 4096], P(None, 'dp'), may hold values from 0.1 to 1.9
- w_query: bfloat16 [2, 4096, 4096], P(None, 'tp', 'dp'), may hold values from -0.09375 to 0.09375
- w_key: bfloat16 [2, 4096, 4096], P(None, 'tp', 'dp'), may hold values from -0.09375 to 0.09375
- w_value: bfloat16 [2, 4096, 4096], P(None, 'tp', 'dp'), may hold values from -0.09375 to 0.09375
- w_outgate: bfloat16 [2, 4096, 4096], P(None, 'tp', 'dp'), may hold values from -0.09375 to 0.09375
- w_igate: bfloat16 [2, 4096, 16], replicated, may hold values from -0.09375 to 0.09375
- w_fgate: bfloat16 [2, 4096, 16], replicated, may hold values from -0.09375 to 0.09375
- forget_bias: float32 [2, 16], replicated, may hold values from -1 to 4
- head_gain: float32 [2, 4096], P(None, 'tp'), may hold values from 0.1 to 1.9
- w_proj: bfloat16 [2, 4096, 4096], P(None, 'tp', 'dp'), may hold values from -0.125 to 0.125
- mem_matrix: float32 [2, 24, 4096, 256], P(None, 'dp', 'tp'), may hold values from -0.6 to 0.6
- mem_stab: float32 [2, 24, 16], P(None, 'dp'), may hold values from -4 to 4
Outputs:
- residual_out: bfloat16 [24, 4096], P(None, ('dp', 'tp'))
- mem_matrix_new: float32 [2, 24, 4096, 256], P(None, 'dp', 'tp')
- mem_stab_new: float32 [2, 24, 16], P(None, 'dp')
The draws below stay inside these ranges and needn't reach their ends.
All inputs are finite; a program needn't handle non-finite values.
Results may differ from the reference program's by a relative error of at most 0.009.
Values may be sent and summed in bfloat16 or wider, within the bound.
A program may use at most 64 MiB of HBM per device.

```python
import jax
import jax.numpy as jnp
from jax import lax

D = 4096
HEADS = 16
HEAD_DIM = 256
BLOCKS = 2
SEQS = 24
INNER = 4096
N_TP = 16
N_DP = 2


def draw_residual_in(key, part):
    noise_key, row_key, col_key = jax.random.split(key, 3)
    feature = jnp.arange(D)
    block_pos = feature // (D // (N_DP * N_TP))
    dp_frac = (block_pos // N_TP).astype(jnp.float32) / max(N_DP - 1, 1)
    tp_frac = (block_pos % N_TP).astype(jnp.float32) / max(N_TP - 1, 1)
    ramp = jnp.exp(jnp.log(3.0) * (dp_frac + tp_frac - 1.0))
    col_scale = ramp * jnp.exp(jax.random.uniform(col_key, (D,), jnp.float32, jnp.log(0.7), jnp.log(1.4)))
    row_scale = jnp.exp(jax.random.uniform(row_key, (SEQS,), jnp.float32, jnp.log(0.5), jnp.log(5.0)))
    raw_values = jnp.clip(jax.random.normal(noise_key, (SEQS, D), jnp.float32), -4.0, 4.0)
    shaped = raw_values * row_scale[:, None] * col_scale[None, :]
    return jnp.clip(shaped, -40.0, 40.0).astype(jnp.bfloat16)


def strengthened(values, rng, source, target, shards_of, factor):
    owner, partner = [(jnp.arange(values.shape[axis_at]) // (values.shape[axis_at] // shards_of)).reshape([-1 if axis == axis_at else 1 for axis in range(values.ndim)]) for axis_at in (source, target)]
    chosen = jax.random.permutation(rng, shards_of)[partner]
    strong = (owner == chosen) | (owner == (partner + shards_of // 2) % shards_of)
    return jnp.where(strong, factor * values, values)


def steps_of(rng, dims, shards, low, largest):
    def one(position, parts):
        draws = jax.random.uniform(jax.random.fold_in(jax.random.fold_in(rng, 6), position), (parts,), jnp.float32, low / len(shards), largest / len(shards))
        return jnp.repeat(jnp.exp(draws), dims[position] // parts).reshape((-1,) + (1,) * (len(dims) - position - 1))

    factor_of = one(*shards[0])
    for cut in shards[1:]:
        factor_of = factor_of * one(*cut)
    return factor_of


def scatter_about(key, shape, deviation, limit, cuts=(), kind=jnp.bfloat16):
    gain = steps_of(key, shape, cuts, -0.22, 0.18) if cuts else 1.0
    entries = jax.random.normal(key, shape, jnp.float32) * deviation * gain
    return jnp.minimum(jnp.maximum(entries, -limit), limit).astype(kind)


def bell_draw_with(rng, extent, width, most, cuts, heavy, held_as=jnp.bfloat16):
    array = width * jax.random.normal(rng, extent, jnp.float32)
    if cuts:
        array = array * steps_of(rng, extent, cuts, -0.22, 0.18)
    return jnp.clip(strengthened(array, jax.random.fold_in(rng, 3), *heavy), -most, most).astype(held_as)


def setup_inputs(seed: int = 0) -> dict:
    key_list = jax.random.split(jax.random.key(seed), 14)
    residual_in = draw_residual_in(jax.random.fold_in(key_list[13], 71), 0)
    norm_gain = jnp.clip(1.0 + 0.18 * jax.random.normal(key_list[1], (BLOCKS, D), jnp.float32), 0.1, 1.9)
    w_query = scatter_about(key_list[2], (BLOCKS, INNER, D), D ** -0.5, 0.09375, ((1, 16), (2, 2)))
    w_key = scatter_about(key_list[3], (BLOCKS, INNER, D), D ** -0.5, 0.09375, ((1, 16), (2, 2)))
    w_value = scatter_about(key_list[4], (BLOCKS, INNER, D), D ** -0.5, 0.09375, ((1, 16), (2, 2)))
    w_outgate = scatter_about(key_list[5], (BLOCKS, INNER, D), D ** -0.5, 0.09375, ((1, 16), (2, 2)))
    w_igate = scatter_about(key_list[6], (BLOCKS, D, HEADS), D ** -0.5, 0.09375)
    w_fgate = scatter_about(key_list[7], (BLOCKS, D, HEADS), D ** -0.5, 0.09375)
    forget_bias = jnp.clip(jax.random.uniform(key_list[8], (BLOCKS, HEADS), jnp.float32, -1.0, 4.0), -1.0, 4.0)
    head_gain = jnp.clip(1.0 + 0.18 * jax.random.normal(key_list[9], (BLOCKS, INNER), jnp.float32), 0.1, 1.9)
    w_proj = bell_draw_with(key_list[10], (BLOCKS, INNER, D), INNER ** -0.5, 0.125, ((1, 16), (2, 2)), (1, 2, 16, 2.0))
    mem_matrix = scatter_about(key_list[11], (BLOCKS, SEQS, INNER, HEAD_DIM), 0.1, 0.6, ((1, 2), (2, 16)), jnp.float32)
    mem_stab = scatter_about(key_list[12], (BLOCKS, SEQS, HEADS), 1.0, 4.0, ((1, 2),), jnp.float32)
    return {"residual_in": residual_in, "norm_gain": norm_gain, "w_query": w_query, "w_key": w_key, "w_value": w_value, "w_outgate": w_outgate, "w_igate": w_igate, "w_fgate": w_fgate, "forget_bias": forget_bias, "head_gain": head_gain, "w_proj": w_proj, "mem_matrix": mem_matrix, "mem_stab": mem_stab}


epsilon = 1e-06

def memory_block(layer_input, norm_gain, w_query, w_key, w_value, w_outgate, w_igate, w_fgate, forget_bias, head_gain, w_proj, mem_matrix, mem_stab):
    seq_count = layer_input.shape[0]
    head_count = w_igate.shape[1]
    inner_width = w_query.shape[0]
    head_dim = inner_width // head_count
    inputs_f = layer_input.astype(jnp.float32)
    inv_rms = lax.rsqrt(lax.optimization_barrier(jnp.mean(inputs_f * inputs_f, axis=1)) + epsilon)[:, None]
    scaled = (inputs_f * norm_gain[None, :]).astype(jnp.bfloat16)
    query_cols = inv_rms * jnp.dot(scaled, w_query.T, preferred_element_type=jnp.float32)
    key_cols = inv_rms * jnp.dot(scaled, w_key.T, preferred_element_type=jnp.float32) * HEAD_DIM ** (-0.5)
    value_cols = inv_rms * jnp.dot(scaled, w_value.T, preferred_element_type=jnp.float32)
    outgate = inv_rms * jnp.dot(scaled, w_outgate.T, preferred_element_type=jnp.float32)
    in_gate = inv_rms * jnp.dot(scaled, w_igate, preferred_element_type=jnp.float32)
    log_forget = jax.nn.log_sigmoid(inv_rms * jnp.dot(scaled, w_fgate, preferred_element_type=jnp.float32) + forget_bias[None, :])
    stab_new = jnp.maximum(log_forget + mem_stab, in_gate)
    keep_weight = jnp.exp(log_forget + mem_stab - stab_new)
    admit_weight = jnp.exp(in_gate - stab_new)
    key_heads = key_cols.reshape(seq_count, head_count, head_dim)
    value_heads = value_cols.reshape(seq_count, head_count, head_dim)
    previous = mem_matrix.reshape(seq_count, head_count, head_dim, head_dim)
    matrix = keep_weight[:, :, None, None] * previous + admit_weight[:, :, None, None] * value_heads[:, :, :, None] * key_heads[:, :, None, :]
    readout = jnp.einsum('bha,bhca->bhc', query_cols.reshape(seq_count, head_count, head_dim), matrix, precision=lax.Precision.HIGHEST)
    normed = readout * lax.rsqrt(lax.optimization_barrier(jnp.mean(readout * readout, axis=2, keepdims=True)) + epsilon) * head_gain.reshape(head_count, head_dim)[None, :, :]
    gated_out = (jax.nn.sigmoid(outgate) * normed.reshape(seq_count, inner_width)).astype(jnp.bfloat16)
    result = (inputs_f + jnp.dot(gated_out, w_proj, preferred_element_type=jnp.float32)).astype(jnp.bfloat16)
    return (result, matrix.reshape(seq_count, inner_width, head_dim), stab_new)

def reference(residual_in, norm_gain, w_query, w_key, w_value, w_outgate, w_igate, w_fgate, forget_bias, head_gain, w_proj, mem_matrix, mem_stab):
    current = residual_in
    matrices = []
    stabs = []
    for layer_index in range(BLOCKS):
        current, matrix, stab_new = memory_block(current, norm_gain[layer_index], w_query[layer_index], w_key[layer_index], w_value[layer_index], w_outgate[layer_index], w_igate[layer_index], w_fgate[layer_index], forget_bias[layer_index], head_gain[layer_index], w_proj[layer_index], mem_matrix[layer_index], mem_stab[layer_index])
        matrices.append(matrix)
        stabs.append(stab_new)
    return (current, jnp.stack(matrices), jnp.stack(stabs))
```

```python
import functools

import jax
import jax.numpy as jnp
from jax import lax
from jax.experimental import pallas as pl
from jax.experimental.pallas import tpu as pltpu
from jax.sharding import PartitionSpec as P

D = 4096
HEAD_DIM = 256
BLOCKS = 2


epsilon = 1e-06


def swapped(block, axis, apart):
    count = lax.axis_size(axis)
    route = []
    for low in range(count):
        high = low | 1 << apart
        if high != low and high < count:
            route += [(low, high), (high, low)]
    return lax.ppermute(block, axis, route)


def gather_rows(own_rows):
    return lax.all_gather(own_rows, "tp", axis=1, tiled=True)


def finish_block(own_rows, partial_value):
    summed = lax.psum_scatter(partial_value, "tp", scatter_dimension=1, tiled=True)
    return (own_rows.astype(jnp.float32) + summed).astype(jnp.bfloat16)


def project_rows(scaled, weight_cols):
    return lax.dot_general(
        scaled, weight_cols, (((1,), (1,)), ((), ())), preferred_element_type=jnp.float32
    )


def memory_cell(
    layer_index,
    full_rows,
    norm_gain,
    w_query,
    w_key,
    w_value,
    w_outgate,
    w_igate,
    w_fgate,
    forget_bias,
    head_gain,
    w_proj,
    mem_matrix,
    mem_stab,
):
    tp_place = lax.axis_index("tp")
    dp_place = lax.axis_index("dp")
    col_width = w_query.shape[1]
    row_span = w_query.shape[2]
    group_size = HEAD_DIM // col_width
    head_index = tp_place // group_size
    rows_f = full_rows.astype(jnp.float32)
    scaled = (rows_f * norm_gain[layer_index][None, :]).astype(jnp.bfloat16)
    query_part = project_rows(scaled, w_query[layer_index])
    key_part = project_rows(scaled, w_key[layer_index])
    value_part = project_rows(scaled, w_value[layer_index])
    outgate_part = project_rows(scaled, w_outgate[layer_index])
    igate_rows = lax.dynamic_slice_in_dim(w_igate[layer_index], dp_place * row_span, row_span, 0)
    fgate_rows = lax.dynamic_slice_in_dim(w_fgate[layer_index], dp_place * row_span, row_span, 0)
    in_part = jnp.dot(scaled, igate_rows, preferred_element_type=jnp.float32)
    forget_part = jnp.dot(scaled, fgate_rows, preferred_element_type=jnp.float32)
    squares = jnp.sum(rows_f * rows_f, axis=1)
    query_cols, key_cols, value_cols, outgate, in_pre, forget_pre, square_sum = (
        lax.psum_scatter(query_part, "dp", scatter_dimension=0, tiled=True),
        lax.psum_scatter(key_part, "dp", scatter_dimension=0, tiled=True),
        lax.psum_scatter(value_part, "dp", scatter_dimension=0, tiled=True),
        lax.psum_scatter(outgate_part, "dp", scatter_dimension=0, tiled=True),
        lax.psum_scatter(in_part, "dp", scatter_dimension=0, tiled=True),
        lax.psum_scatter(forget_part, "dp", scatter_dimension=0, tiled=True),
        lax.psum_scatter(squares, "dp", scatter_dimension=0, tiled=True),
    )
    inv_rms = lax.rsqrt(square_sum / D + epsilon)
    row_scale = inv_rms[:, None]
    query_cols = row_scale * query_cols
    key_cols = row_scale * key_cols * HEAD_DIM ** (-0.5)
    value_cols = row_scale * value_cols
    outgate = row_scale * outgate
    in_gate = row_scale * in_pre
    log_forget = jax.nn.log_sigmoid(row_scale * forget_pre + forget_bias[layer_index][None, :])
    previous = mem_stab[layer_index]
    stab_new = jnp.maximum(log_forget + previous, in_gate)
    keep_weight = jnp.exp(log_forget + previous - stab_new)
    admit_weight = jnp.exp(in_gate - stab_new)
    keep_head = lax.dynamic_slice_in_dim(keep_weight, head_index, 1, 1)
    admit_head = lax.dynamic_slice_in_dim(admit_weight, head_index, 1, 1)
    paired = jnp.stack([query_cols, key_cols])
    for bit_index in range(group_size.bit_length() - 1):
        partner = swapped(paired, "tp", bit_index)
        is_upper = tp_place // (1 << bit_index) % 2 == 1
        paired = jnp.concatenate(
            [jnp.where(is_upper, partner, paired), jnp.where(is_upper, paired, partner)], axis=2
        )
    matrix = (
        keep_head[:, :, None] * mem_matrix[layer_index]
        + admit_head[:, :, None] * value_cols[:, :, None] * paired[1][:, None, :]
    )
    readout = jnp.einsum("bk,bvk->bv", paired[0], matrix, precision=lax.Precision.HIGHEST)
    energy = jnp.sum(readout * readout, axis=1)
    for bit_index in range(group_size.bit_length() - 1):
        energy = energy + swapped(energy, "tp", bit_index)
    normed = (
        readout * lax.rsqrt(energy / HEAD_DIM + epsilon)[:, None] * head_gain[layer_index][None, :]
    )
    gated_out = (jax.nn.sigmoid(outgate) * normed).astype(jnp.bfloat16)
    proj_rows = w_proj[layer_index]
    partial_value = jnp.dot(
        lax.all_gather(gated_out, "dp", axis=0, tiled=True),
        proj_rows,
        preferred_element_type=jnp.float32,
    )
    return (partial_value, matrix, stab_new)


def per_device(
    residual_in,
    norm_gain,
    w_query,
    w_key,
    w_value,
    w_outgate,
    w_igate,
    w_fgate,
    forget_bias,
    head_gain,
    w_proj,
    mem_matrix,
    mem_stab,
):
    own_rows = residual_in
    full_rows = gather_rows(own_rows)
    matrices = []
    stabs = []
    for layer_index in range(BLOCKS):
        partial_value, matrix, stab_new = memory_cell(
            layer_index,
            full_rows,
            norm_gain,
            w_query,
            w_key,
            w_value,
            w_outgate,
            w_igate,
            w_fgate,
            forget_bias,
            head_gain,
            w_proj,
            mem_matrix,
            mem_stab,
        )
        matrices.append(matrix)
        stabs.append(stab_new)
        if layer_index + 1 == BLOCKS:
            own_rows = finish_block(own_rows, partial_value)
        else:
            own_rows = finish_block(own_rows, partial_value)
            full_rows = gather_rows(own_rows)
    return (own_rows, jnp.stack(matrices), jnp.stack(stabs))


MESH = pl.DeviceIdType.MESH
LANES = 128


def flipped(place, count, step):
    if count & (count - 1):
        return lax.rem(place + step, count)
    for bit in range(count.bit_length() - 1):
        if step >> bit & 1:
            place = place + (1 - 2 * (place // (1 << bit) % 2)) * (1 << bit)
    return place


def source_of(place, count, step):
    if count & (count - 1):
        return lax.rem(place + count - step, count)
    return flipped(place, count, step)


def fused_kernel(
    n_tp,
    n_dp,
    seqs,
    residual_ref,
    gain_ref,
    bias_ref,
    head_gain_ref,
    stab_ref,
    wq_hbm,
    wk_hbm,
    wv_hbm,
    wo_hbm,
    wi_hbm,
    wf_hbm,
    wp_hbm,
    mem_hbm,
    out_ref,
    stab_out_ref,
    keep_out_ref,
    value_out_ref,
    key_out_ref,
    w_in,
    w_gate,
    w_out,
    mem,
    mem_low,
    rows,
    scaled_buf,
    partial_buf,
    part_send,
    part_recv,
    gate_send,
    gate_recv,
    gated_all,
    gated_rows,
    sum_send,
    sum_recv,
    w_sem,
    mem_sem,
    rows_send_sem,
    rows_recv_sem,
    part_send_sem,
    part_recv_sem,
    gate_send_sem,
    gate_recv_sem,
    gated_send_sem,
    gated_recv_sem,
    sum_send_sem,
    sum_recv_sem,
):
    me = lax.axis_index("tp")
    core = lax.axis_index("dp")
    width = residual_ref.shape[1]
    share = seqs // n_dp
    head_dim = mem.shape[-1]
    span = n_tp * width
    heads = bias_ref.shape[1]
    pad = part_send.shape[2]

    copies = {}

    def fetch(name, src, dst, sem):
        copies[name] = pltpu.make_async_copy(src, dst, sem)
        copies[name].start()

    def land(name):
        copies.pop(name).wait()

    row_start = pl.multiple_of(core * span, span)
    for j in range(BLOCKS):
        for i, w in enumerate((wq_hbm, wk_hbm, wv_hbm, wo_hbm)):
            fetch(("in", j, i), w.at[j], w_in.at[j, i], w_sem.at[j, i])
        for i, w in enumerate((wi_hbm, wf_hbm)):
            fetch(
                ("gate", j, i), w.at[j, pl.ds(row_start, span)], w_gate.at[j, i], w_sem.at[j, 4 + i]
            )
        fetch(("mem", j), mem_hbm.at[j], mem.at[j], mem_sem.at[j])
        fetch(("out", j), wp_hbm.at[j], w_out.at[j], w_sem.at[j, 6])

    barrier = pltpu.get_barrier_semaphore()
    for step in range(n_tp - 1, 0, -1):
        pl.semaphore_signal(
            barrier, inc=1, device_id={"tp": flipped(me, n_tp, step)}, device_id_type=MESH
        )
    for step in range(1, n_dp):
        pl.semaphore_signal(
            barrier, inc=1, device_id={"dp": flipped(core, n_dp, step)}, device_id_type=MESH
        )
    rows[0, me] = residual_ref[...]
    pl.semaphore_wait(barrier, n_tp - 1 + n_dp - 1)

    own = residual_ref[...].astype(jnp.float32)
    for j in range(BLOCKS):
        sends = []
        for step in range(n_tp - 1, 0, -1):
            copy = pltpu.make_async_remote_copy(
                src_ref=rows.at[j, me],
                dst_ref=rows.at[j, me],
                send_sem=rows_send_sem.at[j, step],
                recv_sem=rows_recv_sem.at[j, step],
                device_id={"tp": flipped(me, n_tp, step)},
                device_id_type=MESH,
            )
            copy.start()
            sends.append(copy)
        land(("mem", j))
        for b in range(share):
            mem_low[j, b] = mem[j, b].astype(jnp.bfloat16)
        for i in range(4):
            land(("in", j, i))
        for i in range(2):
            land(("gate", j, i))
        for copy in sends:
            copy.wait()

        squares = jnp.zeros((seqs, width), jnp.float32)
        for t in range(n_tp):
            chunk = rows[j, t].astype(jnp.float32)
            squares = squares + chunk * chunk
            cols = slice(t * width, (t + 1) * width)
            scaled_buf[:, cols] = (chunk * gain_ref[j : j + 1, cols]).astype(jnp.bfloat16)
        square_sum = jnp.sum(squares, axis=1, keepdims=True)
        scaled = scaled_buf[...]
        cols_in = 4 * head_dim
        for i in range(2):
            partial_buf[:, cols_in + i * LANES : cols_in + i * LANES + heads] = jnp.dot(
                scaled, w_gate[j, i], preferred_element_type=jnp.float32
            )
        partial_buf[:, cols_in + 2 * LANES :] = jnp.broadcast_to(square_sum, (seqs, LANES))
        for i in range(4):
            partial_buf[:, i * head_dim : (i + 1) * head_dim] = lax.dot_general(
                scaled, w_in[j, i], (((1,), (1,)), ((), ())), preferred_element_type=jnp.float32
            )
        for d in range(n_dp):
            mine = partial_buf[d * share : (d + 1) * share, :]
            gate_send[j, d, :share, :] = mine[:, cols_in:]
            part_send[j, d, :share, :] = mine[:, :cols_in].astype(jnp.bfloat16)
        sends = []
        for step in range(1, n_dp):
            target = flipped(core, n_dp, step)
            for src, dst, send_sem, recv_sem in (
                (part_send, part_recv, part_send_sem, part_recv_sem),
                (gate_send, gate_recv, gate_send_sem, gate_recv_sem),
            ):
                copy = pltpu.make_async_remote_copy(
                    src_ref=src.at[j, target],
                    dst_ref=dst.at[j, step],
                    send_sem=send_sem.at[j, step],
                    recv_sem=recv_sem.at[j, step],
                    device_id={"dp": target},
                    device_id_type=MESH,
                )
                copy.start()
                sends.append(copy)
        sums = part_send[j, core, :share, :].astype(jnp.float32)
        gates = gate_send[j, core, :share, :]
        for copy in sends:
            copy.wait()
        for step in range(1, n_dp):
            sums = sums + part_recv[j, step, :share, :].astype(jnp.float32)
            gates = gates + gate_recv[j, step, :share, :]

        inv_rms = lax.rsqrt(gates[:, 2 * LANES : 2 * LANES + 1] / D + epsilon)
        query = inv_rms * sums[:, :head_dim]
        key = inv_rms * sums[:, head_dim : 2 * head_dim] * HEAD_DIM ** (-0.5)
        value = inv_rms * sums[:, 2 * head_dim : 3 * head_dim]
        outgate = inv_rms * sums[:, 3 * head_dim : 4 * head_dim]
        in_gate = inv_rms * gates[:, :heads]
        forget_pre = inv_rms * gates[:, LANES : LANES + heads] + bias_ref[j : j + 1, :]
        log_forget = jnp.minimum(forget_pre, 0.0) - jnp.log1p(jnp.exp(-jnp.abs(forget_pre)))
        previous = stab_ref[j]
        stab_new = jnp.maximum(log_forget + previous, in_gate)
        stab_out_ref[j] = stab_new
        keep_all = jnp.exp(log_forget + previous - stab_new)
        admit_all = jnp.exp(in_gate - stab_new)
        is_head = lax.broadcasted_iota(jnp.int32, (share, heads), 1) == me
        keep = jnp.sum(jnp.where(is_head, keep_all, 0.0), axis=1, keepdims=True)
        admit = jnp.sum(jnp.where(is_head, admit_all, 0.0), axis=1, keepdims=True)
        admitted = admit * value
        keep_out_ref[j] = jnp.broadcast_to(keep, (share, head_dim))
        value_out_ref[j] = admitted
        key_out_ref[j] = key
        query_low = query.astype(jnp.bfloat16)
        row_index = lax.broadcasted_iota(jnp.int32, (share, head_dim), 0)
        recalled = jnp.zeros((share, head_dim), jnp.float32)
        for b in range(share):
            product = lax.dot_general(
                query_low, mem_low[j, b], (((1,), (1,)), ((), ())), preferred_element_type=jnp.float32
            )
            recalled = jnp.where(row_index == b, product, recalled)
        overlap = jnp.sum(query * key, axis=1, keepdims=True)
        readout = keep * recalled + admitted * overlap
        energy = jnp.sum(readout * readout, axis=1, keepdims=True)
        normed = readout * lax.rsqrt(energy / HEAD_DIM + epsilon) * head_gain_ref[j : j + 1, :]
        gated = normed / (1.0 + jnp.exp(-outgate))
        gated_all[j, core, :share, :] = gated.astype(jnp.bfloat16)
        sends = []
        for step in range(1, n_dp):
            copy = pltpu.make_async_remote_copy(
                src_ref=gated_all.at[j, core],
                dst_ref=gated_all.at[j, core],
                send_sem=gated_send_sem.at[j, step],
                recv_sem=gated_recv_sem.at[j, step],
                device_id={"dp": flipped(core, n_dp, step)},
                device_id_type=MESH,
            )
            copy.start()
            sends.append(copy)
        land(("out", j))
        for copy in sends:
            copy.wait()
        for d in range(n_dp):
            gated_rows[d * share : (d + 1) * share, :] = gated_all[j, d, :share, :].astype(jnp.float32)
        gated_low = gated_rows[...].astype(jnp.bfloat16)
        block_cols = 2 * width
        for c in range(span // block_cols):
            product = jnp.dot(
                gated_low,
                w_out[j, :, c * block_cols : (c + 1) * block_cols],
                preferred_element_type=jnp.float32,
            )
            for part in range(2):
                sum_send[j, 2 * c + part] = product[:, part * width : (part + 1) * width].astype(
                    jnp.bfloat16
                )
        sends = []
        for step in range(n_tp - 1, 0, -1):
            target = flipped(me, n_tp, step)
            copy = pltpu.make_async_remote_copy(
                src_ref=sum_send.at[j, target],
                dst_ref=sum_recv.at[j, step],
                send_sem=sum_send_sem.at[j, step],
                recv_sem=sum_recv_sem.at[j, step],
                device_id={"tp": target},
                device_id_type=MESH,
            )
            copy.start()
            sends.append(copy)
        total = sum_send[j, me].astype(jnp.float32)
        for copy in sends:
            copy.wait()
        for step in range(1, n_tp):
            total = total + sum_recv[j, step].astype(jnp.float32)
        rounded = (own + total).astype(jnp.bfloat16)
        if j + 1 < BLOCKS:
            rows[j + 1, me] = rounded
            own = rounded.astype(jnp.float32)
        else:
            out_ref[...] = rounded


def fused_device(n_tp, n_dp, residual_in, norm_gain, w_query, w_key, w_value, w_outgate, w_igate,
                 w_fgate, forget_bias, head_gain, w_proj, mem_matrix, mem_stab):
    seqs, width = residual_in.shape
    _, head_dim, span = w_query.shape
    heads = w_igate.shape[2]
    share = seqs // n_dp
    pad = -(-share // 16) * 16
    low, wide = jnp.bfloat16, jnp.float32
    in_vmem = pl.BlockSpec(memory_space=pltpu.VMEM)
    in_hbm = pl.BlockSpec(memory_space=pl.ANY)
    per_block = lambda shape, dtype: pltpu.VMEM((BLOCKS,) + shape, dtype)
    sems = lambda count: pltpu.SemaphoreType.DMA((BLOCKS, count))
    out, stab_new, keep, value, key = pl.pallas_call(
        functools.partial(fused_kernel, n_tp, n_dp, seqs),
        out_shape=(
            jax.ShapeDtypeStruct((seqs, width), low),
            jax.ShapeDtypeStruct((BLOCKS, share, heads), wide),
            jax.ShapeDtypeStruct((BLOCKS, share, head_dim), wide),
            jax.ShapeDtypeStruct((BLOCKS, share, head_dim), wide),
            jax.ShapeDtypeStruct((BLOCKS, share, head_dim), wide),
        ),
        in_specs=[in_vmem] * 5 + [in_hbm] * 8,
        out_specs=[in_vmem] * 5,
        scratch_shapes=[
            per_block((4, head_dim, span), low),
            per_block((2, span, heads), low),
            per_block((head_dim, span), low),
            per_block((share, head_dim, head_dim), wide),
            per_block((share, head_dim, head_dim), low),
            per_block((n_tp, seqs, width), low),
            pltpu.VMEM((seqs, span), low),
            pltpu.VMEM((seqs, 4 * head_dim + 3 * LANES), wide),
            per_block((n_dp, pad, 4 * head_dim), low),
            per_block((n_dp, pad, 4 * head_dim), low),
            per_block((n_dp, pad, 3 * LANES), wide),
            per_block((n_dp, pad, 3 * LANES), wide),
            per_block((n_dp, pad, head_dim), low),
            pltpu.VMEM((seqs, head_dim), wide),
            per_block((n_tp, seqs, width), low),
            per_block((n_tp, seqs, width), low),
            sems(7),
            pltpu.SemaphoreType.DMA((BLOCKS,)),
            sems(n_tp),
            sems(n_tp),
            sems(n_dp),
            sems(n_dp),
            sems(n_dp),
            sems(n_dp),
            sems(n_dp),
            sems(n_dp),
            sems(n_tp),
            sems(n_tp),
        ],
        compiler_params=pltpu.CompilerParams(collective_id=0, has_side_effects=True),
        name="both_blocks",
    )(
        residual_in, norm_gain, forget_bias, head_gain, mem_stab,
        w_query, w_key, w_value, w_outgate, w_igate, w_fgate, w_proj, mem_matrix,
    )
    matrix = (
        keep[:, :, None, :] * mem_matrix + value[:, :, :, None] * key[:, :, None, :]
    )
    return out, matrix, stab_new


def solution(mesh):
    in_specs = (
        P(None, ("dp", "tp")),
        P(None, "dp"),
        P(None, "tp", "dp"),
        P(None, "tp", "dp"),
        P(None, "tp", "dp"),
        P(None, "tp", "dp"),
        P(),
        P(),
        P(),
        P(None, "tp"),
        P(None, "tp", "dp"),
        P(None, "dp", "tp", None),
        P(None, "dp", None),
    )
    out_specs = (P(None, ("dp", "tp")), P(None, "dp", "tp", None), P(None, "dp", None))
    n_tp, n_dp = mesh.shape["tp"], mesh.shape["dp"]

    def fits(residual_in, w_query):
        width = residual_in.shape[1] // (n_tp * n_dp)
        return (
            w_query.shape[1] == n_tp * HEAD_DIM
            and width % LANES == 0
            and n_tp % 2 == 0
            and residual_in.shape[0] % n_dp == 0
        )

    def run(residual_in, norm_gain, w_query, *others):
        if fits(residual_in, w_query):
            body = functools.partial(fused_device, n_tp, n_dp)
        else:
            body = per_device
        step = jax.shard_map(
            body, mesh=mesh, in_specs=in_specs, out_specs=out_specs, check_vma=False
        )
        return step(residual_in, norm_gain, w_query, *others)

    return run
```

```python
import functools

import jax
import jax.numpy as jnp
from jax import lax
from jax.experimental import pallas as pl
from jax.experimental.pallas import tpu as pltpu
from jax.sharding import PartitionSpec as P

D = 4096
HEAD_DIM = 256
BLOCKS = 2


epsilon = 1e-06


def swapped(block, axis, apart):
    count = lax.axis_size(axis)
    route = []
    for low in range(count):
        high = low | 1 << apart
        if high != low and high < count:
            route += [(low, high), (high, low)]
    return lax.ppermute(block, axis, route)


def gather_rows(own_rows):
    return lax.all_gather(own_rows, "tp", axis=1, tiled=True)


def finish_block(own_rows, partial_value):
    summed = lax.psum_scatter(partial_value, "tp", scatter_dimension=1, tiled=True)
    return (own_rows.astype(jnp.float32) + summed).astype(jnp.bfloat16)


def project_rows(scaled, weight_cols):
    return lax.dot_general(
        scaled, weight_cols, (((1,), (1,)), ((), ())), preferred_element_type=jnp.float32
    )


def memory_cell(
    layer_index,
    full_rows,
    norm_gain,
    w_query,
    w_key,
    w_value,
    w_outgate,
    w_igate,
    w_fgate,
    forget_bias,
    head_gain,
    w_proj,
    mem_matrix,
    mem_stab,
):
    tp_place = lax.axis_index("tp")
    dp_place = lax.axis_index("dp")
    col_width = w_query.shape[1]
    row_span = w_query.shape[2]
    group_size = HEAD_DIM // col_width
    head_index = tp_place // group_size
    rows_f = full_rows.astype(jnp.float32)
    scaled = (rows_f * norm_gain[layer_index][None, :]).astype(jnp.bfloat16)
    query_part = project_rows(scaled, w_query[layer_index])
    key_part = project_rows(scaled, w_key[layer_index])
    value_part = project_rows(scaled, w_value[layer_index])
    outgate_part = project_rows(scaled, w_outgate[layer_index])
    igate_rows = lax.dynamic_slice_in_dim(w_igate[layer_index], dp_place * row_span, row_span, 0)
    fgate_rows = lax.dynamic_slice_in_dim(w_fgate[layer_index], dp_place * row_span, row_span, 0)
    in_part = jnp.dot(scaled, igate_rows, preferred_element_type=jnp.float32)
    forget_part = jnp.dot(scaled, fgate_rows, preferred_element_type=jnp.float32)
    squares = jnp.sum(rows_f * rows_f, axis=1)
    query_cols, key_cols, value_cols, outgate, in_pre, forget_pre, square_sum = (
        lax.psum_scatter(query_part, "dp", scatter_dimension=0, tiled=True),
        lax.psum_scatter(key_part, "dp", scatter_dimension=0, tiled=True),
        lax.psum_scatter(value_part, "dp", scatter_dimension=0, tiled=True),
        lax.psum_scatter(outgate_part, "dp", scatter_dimension=0, tiled=True),
        lax.psum_scatter(in_part, "dp", scatter_dimension=0, tiled=True),
        lax.psum_scatter(forget_part, "dp", scatter_dimension=0, tiled=True),
        lax.psum_scatter(squares, "dp", scatter_dimension=0, tiled=True),
    )
    inv_rms = lax.rsqrt(square_sum / D + epsilon)
    row_scale = inv_rms[:, None]
    query_cols = row_scale * query_cols
    key_cols = row_scale * key_cols * HEAD_DIM ** (-0.5)
    value_cols = row_scale * value_cols
    outgate = row_scale * outgate
    in_gate = row_scale * in_pre
    log_forget = jax.nn.log_sigmoid(row_scale * forget_pre + forget_bias[layer_index][None, :])
    previous = mem_stab[layer_index]
    stab_new = jnp.maximum(log_forget + previous, in_gate)
    keep_weight = jnp.exp(log_forget + previous - stab_new)
    admit_weight = jnp.exp(in_gate - stab_new)
    keep_head = lax.dynamic_slice_in_dim(keep_weight, head_index, 1, 1)
    admit_head = lax.dynamic_slice_in_dim(admit_weight, head_index, 1, 1)
    paired = jnp.stack([query_cols, key_cols])
    for bit_index in range(group_size.bit_length() - 1):
        partner = swapped(paired, "tp", bit_index)
        is_upper = tp_place // (1 << bit_index) % 2 == 1
        paired = jnp.concatenate(
            [jnp.where(is_upper, partner, paired), jnp.where(is_upper, paired, partner)], axis=2
        )
    matrix = (
        keep_head[:, :, None] * mem_matrix[layer_index]
        + admit_head[:, :, None] * value_cols[:, :, None] * paired[1][:, None, :]
    )
    readout = jnp.einsum("bk,bvk->bv", paired[0], matrix, precision=lax.Precision.HIGHEST)
    energy = jnp.sum(readout * readout, axis=1)
    for bit_index in range(group_size.bit_length() - 1):
        energy = energy + swapped(energy, "tp", bit_index)
    normed = (
        readout * lax.rsqrt(energy / HEAD_DIM + epsilon)[:, None] * head_gain[layer_index][None, :]
    )
    gated_out = (jax.nn.sigmoid(outgate) * normed).astype(jnp.bfloat16)
    proj_rows = w_proj[layer_index]
    partial_value = jnp.dot(
        lax.all_gather(gated_out, "dp", axis=0, tiled=True),
        proj_rows,
        preferred_element_type=jnp.float32,
    )
    return (partial_value, matrix, stab_new)


def per_device(
    residual_in,
    norm_gain,
    w_query,
    w_key,
    w_value,
    w_outgate,
    w_igate,
    w_fgate,
    forget_bias,
    head_gain,
    w_proj,
    mem_matrix,
    mem_stab,
):
    own_rows = residual_in
    full_rows = gather_rows(own_rows)
    matrices = []
    stabs = []
    for layer_index in range(BLOCKS):
        partial_value, matrix, stab_new = memory_cell(
            layer_index,
            full_rows,
            norm_gain,
            w_query,
            w_key,
            w_value,
            w_outgate,
            w_igate,
            w_fgate,
            forget_bias,
            head_gain,
            w_proj,
            mem_matrix,
            mem_stab,
        )
        matrices.append(matrix)
        stabs.append(stab_new)
        if layer_index + 1 == BLOCKS:
            own_rows = finish_block(own_rows, partial_value)
        else:
            own_rows = finish_block(own_rows, partial_value)
            full_rows = gather_rows(own_rows)
    return (own_rows, jnp.stack(matrices), jnp.stack(stabs))


MESH = pl.DeviceIdType.MESH
LANES = 128


def flipped(place, count, step):
    if count & (count - 1):
        return lax.rem(place + step, count)
    for bit in range(count.bit_length() - 1):
        if step >> bit & 1:
            place = place + (1 - 2 * (place // (1 << bit) % 2)) * (1 << bit)
    return place


def fused_kernel(
    n_tp,
    n_dp,
    seqs,
    residual_ref,
    gain_ref,
    bias_ref,
    head_gain_ref,
    stab_ref,
    wq_hbm,
    wk_hbm,
    wv_hbm,
    wo_hbm,
    wi_hbm,
    wf_hbm,
    wp_hbm,
    mem_hbm,
    out_ref,
    stab_out_ref,
    keep_out_ref,
    value_out_ref,
    key_out_ref,
    w_in,
    w_gate,
    w_out,
    mem,
    mem_low,
    rows,
    partial_buf,
    part_send,
    part_recv,
    gate_send,
    gate_recv,
    gated_all,
    gated_rows,
    sum_send,
    sum_recv,
    w_sem,
    mem_sem,
    rows_send_sem,
    rows_recv_sem,
    part_send_sem,
    part_recv_sem,
    gate_send_sem,
    gate_recv_sem,
    gated_send_sem,
    gated_recv_sem,
    sum_send_sem,
    sum_recv_sem,
):
    me = lax.axis_index("tp")
    core = lax.axis_index("dp")
    width = residual_ref.shape[1]
    share = seqs // n_dp
    head_dim = mem.shape[-1]
    span = n_tp * width
    heads = bias_ref.shape[1]

    copies = {}

    def fetch(name, src, dst, sem):
        copies[name] = pltpu.make_async_copy(src, dst, sem)
        copies[name].start()

    def land(name):
        copies.pop(name).wait()

    row_start = pl.multiple_of(core * span, span)
    for j in range(BLOCKS):
        for i, w in enumerate((wq_hbm, wk_hbm, wv_hbm, wo_hbm)):
            fetch(("in", j, i), w.at[j], w_in.at[j, i], w_sem.at[j, i])
        for i, w in enumerate((wi_hbm, wf_hbm)):
            fetch(
                ("gate", j, i),
                w.at[j, :, pl.ds(row_start, span)],
                w_gate.at[j, pl.ds(i * heads, heads)],
                w_sem.at[j, 4 + i],
            )
        fetch(("mem", j), mem_hbm.at[j], mem.at[j], mem_sem.at[j])
        fetch(("out", j), wp_hbm.at[j], w_out.at[j], w_sem.at[j, 6])

    barrier = pltpu.get_barrier_semaphore()
    for step in range(n_tp - 1, 0, -1):
        pl.semaphore_signal(
            barrier, inc=1, device_id={"tp": flipped(me, n_tp, step)}, device_id_type=MESH
        )
    for step in range(1, n_dp):
        pl.semaphore_signal(
            barrier, inc=1, device_id={"dp": flipped(core, n_dp, step)}, device_id_type=MESH
        )
    rows[0, me] = residual_ref[...]
    pl.semaphore_wait(barrier, n_tp - 1 + n_dp - 1)

    own = residual_ref[...].astype(jnp.float32)
    late_sends = []
    for j in range(BLOCKS):
        gather = {}
        for step in range(n_tp - 1, 0, -1):
            gather[step] = pltpu.make_async_remote_copy(
                src_ref=rows.at[j, me],
                dst_ref=rows.at[j, me],
                send_sem=rows_send_sem.at[j, step],
                recv_sem=rows_recv_sem.at[j, step],
                device_id={"tp": flipped(me, n_tp, step)},
                device_id_type=MESH,
            )
            gather[step].start()
        land(("mem", j))
        for b in range(share):
            mem_low[j, b] = mem[j, b].astype(jnp.bfloat16)
        for i in range(4):
            land(("in", j, i))
        for i in range(2):
            land(("gate", j, i))
        squares = jnp.zeros((seqs, 2 * width), jnp.float32)
        gate_sum = jnp.zeros((seqs, 2 * heads), jnp.float32)
        in_sums = [jnp.zeros((seqs, head_dim), jnp.float32)] * 4
        for step in range(n_tp // 2):
            pair = flipped(me // 2, n_tp // 2, step)
            for arrived in (2 * step, 2 * step + 1):
                if arrived:
                    gather[arrived].wait_recv()
            chunk = jnp.concatenate([rows[j, 2 * pair], rows[j, 2 * pair + 1]], axis=1)
            chunk = chunk.astype(jnp.float32)
            squares = squares + chunk * chunk
            cols = pl.ds(pl.multiple_of(pair * 2 * width, 2 * width), 2 * width)
            scaled = (chunk * gain_ref[j : j + 1, cols]).astype(jnp.bfloat16)
            gate_sum = gate_sum + project_rows(scaled, w_gate[j, :, cols])
            for i in range(4):
                in_sums[i] = in_sums[i] + project_rows(scaled, w_in[j, i, :, cols])
        cols_in = 4 * head_dim
        square_sum = jnp.sum(squares, axis=1, keepdims=True)
        partial_buf[:, cols_in:] = jnp.broadcast_to(square_sum, (seqs, LANES))
        partial_buf[:, cols_in : cols_in + 2 * heads] = gate_sum
        for i in range(4):
            partial_buf[:, i * head_dim : (i + 1) * head_dim] = in_sums[i]
        for d in range(n_dp):
            mine = partial_buf[d * share : (d + 1) * share, :]
            gate_send[j, d, :share, :] = mine[:, cols_in:]
            part_send[j, d, :share, :] = mine[:, :cols_in].astype(jnp.bfloat16)
        sends = []
        for step in range(1, n_dp):
            target = flipped(core, n_dp, step)
            for src, dst, send_sem, recv_sem in (
                (part_send, part_recv, part_send_sem, part_recv_sem),
                (gate_send, gate_recv, gate_send_sem, gate_recv_sem),
            ):
                copy = pltpu.make_async_remote_copy(
                    src_ref=src.at[j, target],
                    dst_ref=dst.at[j, step],
                    send_sem=send_sem.at[j, step],
                    recv_sem=recv_sem.at[j, step],
                    device_id={"dp": target},
                    device_id_type=MESH,
                )
                copy.start()
                sends.append(copy)
        sums = part_send[j, core, :share, :].astype(jnp.float32)
        gates = gate_send[j, core, :share, :]
        for copy in sends:
            copy.wait()
        for step in range(1, n_dp):
            sums = sums + part_recv[j, step, :share, :].astype(jnp.float32)
            gates = gates + gate_recv[j, step, :share, :]

        inv_rms = lax.rsqrt(gates[:, 2 * heads : 2 * heads + 1] / D + epsilon)
        query = inv_rms * sums[:, :head_dim]
        key = inv_rms * sums[:, head_dim : 2 * head_dim] * HEAD_DIM ** (-0.5)
        value = inv_rms * sums[:, 2 * head_dim : 3 * head_dim]
        outgate = inv_rms * sums[:, 3 * head_dim : 4 * head_dim]
        in_gate = inv_rms * gates[:, :heads]
        forget_pre = inv_rms * gates[:, heads : 2 * heads] + bias_ref[j : j + 1, :]
        log_forget = jnp.minimum(forget_pre, 0.0) - jnp.log1p(jnp.exp(-jnp.abs(forget_pre)))
        previous = stab_ref[:, j, :]
        stab_new = jnp.maximum(log_forget + previous, in_gate)
        stab_out_ref[:, j, :] = stab_new
        keep_all = jnp.exp(log_forget + previous - stab_new)
        admit_all = jnp.exp(in_gate - stab_new)
        is_head = lax.broadcasted_iota(jnp.int32, (share, heads), 1) == me
        keep = jnp.sum(jnp.where(is_head, keep_all, 0.0), axis=1, keepdims=True)
        admit = jnp.sum(jnp.where(is_head, admit_all, 0.0), axis=1, keepdims=True)
        admitted = admit * value
        keep_out_ref[j] = jnp.broadcast_to(keep, (share, head_dim))
        value_out_ref[j] = admitted
        key_out_ref[j] = key
        query_low = query.astype(jnp.bfloat16)
        row_index = lax.broadcasted_iota(jnp.int32, (share, head_dim), 0)
        recalled = jnp.zeros((share, head_dim), jnp.float32)
        for b in range(share):
            product = lax.dot_general(
                query_low, mem_low[j, b], (((1,), (1,)), ((), ())), preferred_element_type=jnp.float32
            )
            recalled = jnp.where(row_index == b, product, recalled)
        overlap = jnp.sum(query * key, axis=1, keepdims=True)
        readout = keep * recalled + admitted * overlap
        energy = jnp.sum(readout * readout, axis=1, keepdims=True)
        normed = readout * lax.rsqrt(energy / HEAD_DIM + epsilon) * head_gain_ref[j : j + 1, :]
        gated = normed / (1.0 + jnp.exp(-outgate))
        gated_all[j, core, :share, :] = gated.astype(jnp.bfloat16)
        sends = []
        for step in range(1, n_dp):
            copy = pltpu.make_async_remote_copy(
                src_ref=gated_all.at[j, core],
                dst_ref=gated_all.at[j, core],
                send_sem=gated_send_sem.at[j, step],
                recv_sem=gated_recv_sem.at[j, step],
                device_id={"dp": flipped(core, n_dp, step)},
                device_id_type=MESH,
            )
            copy.start()
            sends.append(copy)
        land(("out", j))
        for copy in sends:
            copy.wait()
        for d in range(n_dp):
            gated_rows[d * share : (d + 1) * share, :] = gated_all[j, d, :share, :].astype(jnp.float32)
        gated_low = gated_rows[...].astype(jnp.bfloat16)
        scatter = {}

        def send_pair(step):
            for sent in (2 * step + 1, 2 * step):
                if sent:
                    target = flipped(me, n_tp, sent)
                    scatter[sent] = pltpu.make_async_remote_copy(
                        src_ref=sum_send.at[j, target],
                        dst_ref=sum_recv.at[j, sent],
                        send_sem=sum_send_sem.at[j, sent],
                        recv_sem=sum_recv_sem.at[j, sent],
                        device_id={"tp": target},
                        device_id_type=MESH,
                    )
                    scatter[sent].start()

        for step in range(n_tp // 2 - 1, -1, -1):
            pair = flipped(me // 2, n_tp // 2, step)
            cols = pl.ds(pl.multiple_of(pair * 2 * width, 2 * width), 2 * width)
            product = jnp.dot(gated_low, w_out[j, :, cols], preferred_element_type=jnp.float32)
            for part in range(2):
                sum_send[j, 2 * pair + part] = product[:, part * width : (part + 1) * width].astype(
                    jnp.bfloat16
                )
            if step + 1 < n_tp // 2:
                send_pair(step + 1)
        send_pair(0)
        total = own + sum_send[j, me].astype(jnp.float32)
        for step in range(1, n_tp):
            scatter[step].wait_recv()
            total = total + sum_recv[j, step].astype(jnp.float32)
        late_sends += [*gather.values(), *scatter.values()]
        rounded = total.astype(jnp.bfloat16)
        if j + 1 < BLOCKS:
            rows[j + 1, me] = rounded
            own = rounded.astype(jnp.float32)
        else:
            out_ref[...] = rounded
    for copy in late_sends:
        copy.wait_send()


def fused_device(n_tp, n_dp, residual_in, norm_gain, w_query, w_key, w_value, w_outgate, w_igate,
                 w_fgate, forget_bias, head_gain, w_proj, mem_matrix, mem_stab):
    seqs, width = residual_in.shape
    _, head_dim, span = w_query.shape
    heads = w_igate.shape[2]
    share = seqs // n_dp
    pad = -(-share // 16) * 16
    low, wide = jnp.bfloat16, jnp.float32
    in_vmem = pl.BlockSpec(memory_space=pltpu.VMEM)
    in_hbm = pl.BlockSpec(memory_space=pl.ANY)
    per_block = lambda shape, dtype: pltpu.VMEM((BLOCKS,) + shape, dtype)
    sems = lambda count: pltpu.SemaphoreType.DMA((BLOCKS, count))
    out, stab_new, keep, value, key = pl.pallas_call(
        functools.partial(fused_kernel, n_tp, n_dp, seqs),
        out_shape=(
            jax.ShapeDtypeStruct((seqs, width), low),
            jax.ShapeDtypeStruct((share, BLOCKS, heads), wide),
            jax.ShapeDtypeStruct((BLOCKS, share, head_dim), wide),
            jax.ShapeDtypeStruct((BLOCKS, share, head_dim), wide),
            jax.ShapeDtypeStruct((BLOCKS, share, head_dim), wide),
        ),
        in_specs=[in_vmem] * 5 + [in_hbm] * 8,
        out_specs=[in_vmem] * 5,
        scratch_shapes=[
            per_block((4, head_dim, span), low),
            per_block((2 * heads, span), low),
            per_block((head_dim, span), low),
            per_block((share, head_dim, head_dim), wide),
            per_block((share, head_dim, head_dim), low),
            per_block((n_tp, seqs, width), low),
            pltpu.VMEM((seqs, 4 * head_dim + LANES), wide),
            per_block((n_dp, pad, 4 * head_dim), low),
            per_block((n_dp, pad, 4 * head_dim), low),
            per_block((n_dp, pad, LANES), wide),
            per_block((n_dp, pad, LANES), wide),
            per_block((n_dp, pad, head_dim), low),
            pltpu.VMEM((seqs, head_dim), wide),
            per_block((n_tp, seqs, width), low),
            per_block((n_tp, seqs, width), low),
            sems(7),
            pltpu.SemaphoreType.DMA((BLOCKS,)),
            sems(n_tp),
            sems(n_tp),
            sems(n_dp),
            sems(n_dp),
            sems(n_dp),
            sems(n_dp),
            sems(n_dp),
            sems(n_dp),
            sems(n_tp),
            sems(n_tp),
        ],
        compiler_params=pltpu.CompilerParams(
            collective_id=0, has_side_effects=True
        ),
        cost_estimate=pl.CostEstimate(
            flops=10 * BLOCKS * seqs * head_dim * span,
            bytes_accessed=40 * BLOCKS * head_dim * span,
            transcendentals=0,
        ),
        name="both_blocks",
    )(
        residual_in, norm_gain, forget_bias, head_gain, mem_stab.transpose(1, 0, 2),
        w_query, w_key, w_value, w_outgate, w_igate.swapaxes(1, 2), w_fgate.swapaxes(1, 2),
        w_proj, mem_matrix,
    )
    matrix = (
        keep[:, :, None, :] * mem_matrix + value[:, :, :, None] * key[:, :, None, :]
    )
    return out, matrix, stab_new.transpose(1, 0, 2)


def solution(mesh):
    in_specs = (
        P(None, ("dp", "tp")),
        P(None, "dp"),
        P(None, "tp", "dp"),
        P(None, "tp", "dp"),
        P(None, "tp", "dp"),
        P(None, "tp", "dp"),
        P(),
        P(),
        P(),
        P(None, "tp"),
        P(None, "tp", "dp"),
        P(None, "dp", "tp", None),
        P(None, "dp", None),
    )
    out_specs = (P(None, ("dp", "tp")), P(None, "dp", "tp", None), P(None, "dp", None))
    n_tp, n_dp = mesh.shape["tp"], mesh.shape["dp"]

    def fits(residual_in, w_query, w_igate):
        width = residual_in.shape[1] // (n_tp * n_dp)
        return (
            w_query.shape[1] == n_tp * HEAD_DIM
            and width % LANES == 0
            and n_tp > 1
            and n_tp & (n_tp - 1) == 0
            and w_igate.shape[2] % 16 == 0
            and residual_in.shape[0] % n_dp == 0
        )

    def run(residual_in, norm_gain, w_query, *others):
        if fits(residual_in, w_query, others[3]):
            body = functools.partial(fused_device, n_tp, n_dp)
        else:
            body = per_device
        step = jax.shard_map(
            body, mesh=mesh, in_specs=in_specs, out_specs=out_specs, check_vma=False
        )
        return step(residual_in, norm_gain, w_query, *others)

    return run
```

```python
import functools

import jax
import jax.numpy as jnp
from jax import lax
from jax.experimental import pallas as pl
from jax.experimental.pallas import tpu as pltpu
from jax.sharding import PartitionSpec as P

D = 4096
HEAD_DIM = 256
BLOCKS = 2


epsilon = 1e-06


def swapped(block, axis, apart):
    count = lax.axis_size(axis)
    route = []
    for low in range(count):
        high = low | 1 << apart
        if high != low and high < count:
            route += [(low, high), (high, low)]
    return lax.ppermute(block, axis, route)


def gather_rows(own_rows):
    return lax.all_gather(own_rows, "tp", axis=1, tiled=True)


def finish_block(own_rows, partial_value):
    summed = lax.psum_scatter(partial_value, "tp", scatter_dimension=1, tiled=True)
    return (own_rows.astype(jnp.float32) + summed).astype(jnp.bfloat16)


def project_rows(scaled, weight_cols):
    return lax.dot_general(
        scaled, weight_cols, (((1,), (1,)), ((), ())), preferred_element_type=jnp.float32
    )


def memory_cell(
    layer_index,
    full_rows,
    norm_gain,
    w_query,
    w_key,
    w_value,
    w_outgate,
    w_igate,
    w_fgate,
    forget_bias,
    head_gain,
    w_proj,
    mem_matrix,
    mem_stab,
):
    tp_place = lax.axis_index("tp")
    dp_place = lax.axis_index("dp")
    col_width = w_query.shape[1]
    row_span = w_query.shape[2]
    group_size = HEAD_DIM // col_width
    head_index = tp_place // group_size
    rows_f = full_rows.astype(jnp.float32)
    scaled = (rows_f * norm_gain[layer_index][None, :]).astype(jnp.bfloat16)
    query_part = project_rows(scaled, w_query[layer_index])
    key_part = project_rows(scaled, w_key[layer_index])
    value_part = project_rows(scaled, w_value[layer_index])
    outgate_part = project_rows(scaled, w_outgate[layer_index])
    igate_rows = lax.dynamic_slice_in_dim(w_igate[layer_index], dp_place * row_span, row_span, 0)
    fgate_rows = lax.dynamic_slice_in_dim(w_fgate[layer_index], dp_place * row_span, row_span, 0)
    in_part = jnp.dot(scaled, igate_rows, preferred_element_type=jnp.float32)
    forget_part = jnp.dot(scaled, fgate_rows, preferred_element_type=jnp.float32)
    squares = jnp.sum(rows_f * rows_f, axis=1)
    query_cols, key_cols, value_cols, outgate, in_pre, forget_pre, square_sum = (
        lax.psum_scatter(query_part, "dp", scatter_dimension=0, tiled=True),
        lax.psum_scatter(key_part, "dp", scatter_dimension=0, tiled=True),
        lax.psum_scatter(value_part, "dp", scatter_dimension=0, tiled=True),
        lax.psum_scatter(outgate_part, "dp", scatter_dimension=0, tiled=True),
        lax.psum_scatter(in_part, "dp", scatter_dimension=0, tiled=True),
        lax.psum_scatter(forget_part, "dp", scatter_dimension=0, tiled=True),
        lax.psum_scatter(squares, "dp", scatter_dimension=0, tiled=True),
    )
    inv_rms = lax.rsqrt(square_sum / D + epsilon)
    row_scale = inv_rms[:, None]
    query_cols = row_scale * query_cols
    key_cols = row_scale * key_cols * HEAD_DIM ** (-0.5)
    value_cols = row_scale * value_cols
    outgate = row_scale * outgate
    in_gate = row_scale * in_pre
    log_forget = jax.nn.log_sigmoid(row_scale * forget_pre + forget_bias[layer_index][None, :])
    previous = mem_stab[layer_index]
    stab_new = jnp.maximum(log_forget + previous, in_gate)
    keep_weight = jnp.exp(log_forget + previous - stab_new)
    admit_weight = jnp.exp(in_gate - stab_new)
    keep_head = lax.dynamic_slice_in_dim(keep_weight, head_index, 1, 1)
    admit_head = lax.dynamic_slice_in_dim(admit_weight, head_index, 1, 1)
    paired = jnp.stack([query_cols, key_cols])
    for bit_index in range(group_size.bit_length() - 1):
        partner = swapped(paired, "tp", bit_index)
        is_upper = tp_place // (1 << bit_index) % 2 == 1
        paired = jnp.concatenate(
            [jnp.where(is_upper, partner, paired), jnp.where(is_upper, paired, partner)], axis=2
        )
    matrix = (
        keep_head[:, :, None] * mem_matrix[layer_index]
        + admit_head[:, :, None] * value_cols[:, :, None] * paired[1][:, None, :]
    )
    readout = jnp.einsum("bk,bvk->bv", paired[0], matrix, precision=lax.Precision.HIGHEST)
    energy = jnp.sum(readout * readout, axis=1)
    for bit_index in range(group_size.bit_length() - 1):
        energy = energy + swapped(energy, "tp", bit_index)
    normed = (
        readout * lax.rsqrt(energy / HEAD_DIM + epsilon)[:, None] * head_gain[layer_index][None, :]
    )
    gated_out = (jax.nn.sigmoid(outgate) * normed).astype(jnp.bfloat16)
    proj_rows = w_proj[layer_index]
    partial_value = jnp.dot(
        lax.all_gather(gated_out, "dp", axis=0, tiled=True),
        proj_rows,
        preferred_element_type=jnp.float32,
    )
    return (partial_value, matrix, stab_new)


def per_device(
    residual_in,
    norm_gain,
    w_query,
    w_key,
    w_value,
    w_outgate,
    w_igate,
    w_fgate,
    forget_bias,
    head_gain,
    w_proj,
    mem_matrix,
    mem_stab,
):
    own_rows = residual_in
    full_rows = gather_rows(own_rows)
    matrices = []
    stabs = []
    for layer_index in range(BLOCKS):
        partial_value, matrix, stab_new = memory_cell(
            layer_index,
            full_rows,
            norm_gain,
            w_query,
            w_key,
            w_value,
            w_outgate,
            w_igate,
            w_fgate,
            forget_bias,
            head_gain,
            w_proj,
            mem_matrix,
            mem_stab,
        )
        matrices.append(matrix)
        stabs.append(stab_new)
        if layer_index + 1 == BLOCKS:
            own_rows = finish_block(own_rows, partial_value)
        else:
            own_rows = finish_block(own_rows, partial_value)
            full_rows = gather_rows(own_rows)
    return (own_rows, jnp.stack(matrices), jnp.stack(stabs))


MESH = pl.DeviceIdType.MESH
LANES = 128


def flipped(place, count, step):
    if count & (count - 1):
        return lax.rem(place + step, count)
    for bit in range(count.bit_length() - 1):
        if step >> bit & 1:
            place = place + (1 - 2 * (place // (1 << bit) % 2)) * (1 << bit)
    return place


def fused_kernel(
    n_tp,
    n_dp,
    seqs,
    residual_ref,
    gain_ref,
    bias_ref,
    head_gain_ref,
    stab_ref,
    wq_hbm,
    wk_hbm,
    wv_hbm,
    wo_hbm,
    wi_hbm,
    wf_hbm,
    wp_hbm,
    mem_hbm,
    out_ref,
    stab_out_ref,
    keep_out_ref,
    value_out_ref,
    key_out_ref,
    w_in,
    w_gate,
    w_out,
    mem,
    mem_low,
    rows,
    partial_buf,
    part_send,
    part_recv,
    gate_send,
    gate_recv,
    gated_all,
    gated_rows,
    sum_send,
    sum_recv,
    w_sem,
    mem_sem,
    rows_send_sem,
    rows_recv_sem,
    part_send_sem,
    part_recv_sem,
    gate_send_sem,
    gate_recv_sem,
    gated_send_sem,
    gated_recv_sem,
    sum_send_sem,
    sum_recv_sem,
):
    me = lax.axis_index("tp")
    core = lax.axis_index("dp")
    width = residual_ref.shape[1]
    share = seqs // n_dp
    head_dim = mem.shape[-1]
    span = n_tp * width
    heads = bias_ref.shape[1]

    copies = {}

    def fetch(name, src, dst, sem):
        copies[name] = pltpu.make_async_copy(src, dst, sem)
        copies[name].start()

    def land(name):
        copies.pop(name).wait()

    row_start = pl.multiple_of(core * span, span)

    def fetch_block(j):
        for i, w in enumerate((wq_hbm, wk_hbm, wv_hbm, wo_hbm)):
            fetch(("in", j, i), w.at[j], w_in.at[j, i], w_sem.at[j, i])
        for i, w in enumerate((wi_hbm, wf_hbm)):
            fetch(
                ("gate", j, i),
                w.at[j, :, pl.ds(row_start, span)],
                w_gate.at[j, pl.ds(i * heads, heads)],
                w_sem.at[j, 4 + i],
            )
        fetch(("mem", j), mem_hbm.at[j], mem.at[j], mem_sem.at[j])
        fetch(("out", j), wp_hbm.at[j], w_out.at[j], w_sem.at[j, 6])

    fetch_block(0)
    barrier = pltpu.get_barrier_semaphore()
    for step in range(n_tp - 1, 0, -1):
        pl.semaphore_signal(
            barrier, inc=1, device_id={"tp": flipped(me, n_tp, step)}, device_id_type=MESH
        )
    for step in range(1, n_dp):
        pl.semaphore_signal(
            barrier, inc=1, device_id={"dp": flipped(core, n_dp, step)}, device_id_type=MESH
        )
    rows[0, me] = residual_ref[...]
    pl.semaphore_wait(barrier, n_tp - 1 + n_dp - 1)

    own = residual_ref[...].astype(jnp.float32)
    late_sends = []
    for j in range(BLOCKS):
        gather = {}
        for step in range(n_tp - 1, 0, -1):
            gather[step] = pltpu.make_async_remote_copy(
                src_ref=rows.at[j, me],
                dst_ref=rows.at[j, me],
                send_sem=rows_send_sem.at[j, step],
                recv_sem=rows_recv_sem.at[j, step],
                device_id={"tp": flipped(me, n_tp, step)},
                device_id_type=MESH,
            )
            gather[step].start()
        land(("mem", j))
        for b in range(share):
            mem_low[j, b] = mem[j, b].astype(jnp.bfloat16)
        for i in range(4):
            land(("in", j, i))
        for i in range(2):
            land(("gate", j, i))
        if j + 1 < BLOCKS:
            fetch_block(j + 1)
        squares = jnp.zeros((seqs, 2 * width), jnp.float32)
        gate_sum = jnp.zeros((seqs, 2 * heads), jnp.float32)
        in_sums = [jnp.zeros((seqs, head_dim), jnp.float32)] * 4
        for step in range(n_tp // 2):
            pair = flipped(me // 2, n_tp // 2, step)
            for arrived in (2 * step, 2 * step + 1):
                if arrived:
                    gather[arrived].wait_recv()
            chunk = jnp.concatenate([rows[j, 2 * pair], rows[j, 2 * pair + 1]], axis=1)
            chunk = chunk.astype(jnp.float32)
            squares = squares + chunk * chunk
            cols = pl.ds(pl.multiple_of(pair * 2 * width, 2 * width), 2 * width)
            scaled = (chunk * gain_ref[j : j + 1, cols]).astype(jnp.bfloat16)
            gate_sum = gate_sum + project_rows(scaled, w_gate[j, :, cols])
            for i in range(4):
                in_sums[i] = in_sums[i] + project_rows(scaled, w_in[j, i, :, cols])
        cols_in = 4 * head_dim
        square_sum = jnp.sum(squares, axis=1, keepdims=True)
        partial_buf[:, cols_in:] = jnp.broadcast_to(square_sum, (seqs, LANES))
        partial_buf[:, cols_in : cols_in + 2 * heads] = gate_sum
        for i in range(4):
            partial_buf[:, i * head_dim : (i + 1) * head_dim] = in_sums[i]
        for d in range(n_dp):
            mine = partial_buf[d * share : (d + 1) * share, :]
            gate_send[j, d, :share, :] = mine[:, cols_in:]
            part_send[j, d, :share, :] = mine[:, :cols_in].astype(jnp.bfloat16)
        sends = []
        for step in range(1, n_dp):
            target = flipped(core, n_dp, step)
            for src, dst, send_sem, recv_sem in (
                (part_send, part_recv, part_send_sem, part_recv_sem),
                (gate_send, gate_recv, gate_send_sem, gate_recv_sem),
            ):
                copy = pltpu.make_async_remote_copy(
                    src_ref=src.at[j, target],
                    dst_ref=dst.at[j, step],
                    send_sem=send_sem.at[j, step],
                    recv_sem=recv_sem.at[j, step],
                    device_id={"dp": target},
                    device_id_type=MESH,
                )
                copy.start()
                sends.append(copy)
        sums = part_send[j, core, :share, :].astype(jnp.float32)
        gates = gate_send[j, core, :share, :]
        for copy in sends:
            copy.wait()
        for step in range(1, n_dp):
            sums = sums + part_recv[j, step, :share, :].astype(jnp.float32)
            gates = gates + gate_recv[j, step, :share, :]

        inv_rms = lax.rsqrt(gates[:, 2 * heads : 2 * heads + 1] / D + epsilon)
        query = inv_rms * sums[:, :head_dim]
        key = inv_rms * sums[:, head_dim : 2 * head_dim] * HEAD_DIM ** (-0.5)
        value = inv_rms * sums[:, 2 * head_dim : 3 * head_dim]
        outgate = inv_rms * sums[:, 3 * head_dim : 4 * head_dim]
        in_gate = inv_rms * gates[:, :heads]
        forget_pre = inv_rms * gates[:, heads : 2 * heads] + bias_ref[j : j + 1, :]
        log_forget = jnp.minimum(forget_pre, 0.0) - jnp.log1p(jnp.exp(-jnp.abs(forget_pre)))
        previous = stab_ref[:, j, :]
        stab_new = jnp.maximum(log_forget + previous, in_gate)
        stab_out_ref[:, j, :] = stab_new
        keep_all = jnp.exp(log_forget + previous - stab_new)
        admit_all = jnp.exp(in_gate - stab_new)
        is_head = lax.broadcasted_iota(jnp.int32, (share, heads), 1) == me
        keep = jnp.sum(jnp.where(is_head, keep_all, 0.0), axis=1, keepdims=True)
        admit = jnp.sum(jnp.where(is_head, admit_all, 0.0), axis=1, keepdims=True)
        admitted = admit * value
        keep_out_ref[j] = jnp.broadcast_to(keep, (share, head_dim))
        value_out_ref[j] = admitted
        key_out_ref[j] = key
        query_low = query.astype(jnp.bfloat16)
        row_index = lax.broadcasted_iota(jnp.int32, (share, head_dim), 0)
        recalled = jnp.zeros((share, head_dim), jnp.float32)
        for b in range(share):
            product = lax.dot_general(
                query_low, mem_low[j, b], (((1,), (1,)), ((), ())), preferred_element_type=jnp.float32
            )
            recalled = jnp.where(row_index == b, product, recalled)
        overlap = jnp.sum(query * key, axis=1, keepdims=True)
        readout = keep * recalled + admitted * overlap
        energy = jnp.sum(readout * readout, axis=1, keepdims=True)
        normed = readout * lax.rsqrt(energy / HEAD_DIM + epsilon) * head_gain_ref[j : j + 1, :]
        gated = normed / (1.0 + jnp.exp(-outgate))
        gated_all[j, core, :share, :] = gated.astype(jnp.bfloat16)
        sends = []
        for step in range(1, n_dp):
            copy = pltpu.make_async_remote_copy(
                src_ref=gated_all.at[j, core],
                dst_ref=gated_all.at[j, core],
                send_sem=gated_send_sem.at[j, step],
                recv_sem=gated_recv_sem.at[j, step],
                device_id={"dp": flipped(core, n_dp, step)},
                device_id_type=MESH,
            )
            copy.start()
            sends.append(copy)
        land(("out", j))
        for copy in sends:
            copy.wait()
        for d in range(n_dp):
            gated_rows[d * share : (d + 1) * share, :] = gated_all[j, d, :share, :].astype(jnp.float32)
        gated_low = gated_rows[...].astype(jnp.bfloat16)
        scatter = {}

        def send_pair(step):
            for sent in (2 * step + 1, 2 * step):
                if sent:
                    target = flipped(me, n_tp, sent)
                    scatter[sent] = pltpu.make_async_remote_copy(
                        src_ref=sum_send.at[j, target],
                        dst_ref=sum_recv.at[j, sent],
                        send_sem=sum_send_sem.at[j, sent],
                        recv_sem=sum_recv_sem.at[j, sent],
                        device_id={"tp": target},
                        device_id_type=MESH,
                    )
                    scatter[sent].start()

        for step in range(n_tp // 2 - 1, -1, -1):
            pair = flipped(me // 2, n_tp // 2, step)
            cols = pl.ds(pl.multiple_of(pair * 2 * width, 2 * width), 2 * width)
            product = jnp.dot(gated_low, w_out[j, :, cols], preferred_element_type=jnp.float32)
            for part in range(2):
                sum_send[j, 2 * pair + part] = product[:, part * width : (part + 1) * width].astype(
                    jnp.bfloat16
                )
            if step + 1 < n_tp // 2:
                send_pair(step + 1)
        send_pair(0)
        total = own + sum_send[j, me].astype(jnp.float32)
        for step in range(1, n_tp):
            scatter[step].wait_recv()
            total = total + sum_recv[j, step].astype(jnp.float32)
        late_sends += [*gather.values(), *scatter.values()]
        rounded = total.astype(jnp.bfloat16)
        if j + 1 < BLOCKS:
            rows[j + 1, me] = rounded
            own = rounded.astype(jnp.float32)
        else:
            out_ref[...] = rounded
    for copy in late_sends:
        copy.wait_send()


def update_kernel(
    keep_ref, value_ref, key_ref, mem_ref, out_in, stab_in, mem_out, out_out, stab_out, column_buf
):
    share = keep_ref.shape[1]
    column_buf[...] = jnp.zeros_like(column_buf)
    column_buf[:share, :] = value_ref[0]
    columns = column_buf[...].T
    for b in range(share):
        mem_out[0, b] = (
            keep_ref[0, b : b + 1, :] * mem_ref[0, b]
            + columns[:, b : b + 1] * key_ref[0, b : b + 1, :]
        )
    out_out[...] = out_in[...]
    stab_out[...] = stab_in[...]


def fused_device(n_tp, n_dp, residual_in, norm_gain, w_query, w_key, w_value, w_outgate, w_igate,
                 w_fgate, forget_bias, head_gain, w_proj, mem_matrix, mem_stab):
    seqs, width = residual_in.shape
    _, head_dim, span = w_query.shape
    heads = w_igate.shape[2]
    share = seqs // n_dp
    pad = -(-share // 16) * 16
    low, wide = jnp.bfloat16, jnp.float32
    in_vmem = pl.BlockSpec(memory_space=pltpu.VMEM)
    in_hbm = pl.BlockSpec(memory_space=pl.ANY)
    per_block = lambda shape, dtype: pltpu.VMEM((BLOCKS,) + shape, dtype)
    sems = lambda count: pltpu.SemaphoreType.DMA((BLOCKS, count))
    out, stab_new, keep, value, key = pl.pallas_call(
        functools.partial(fused_kernel, n_tp, n_dp, seqs),
        out_shape=(
            jax.ShapeDtypeStruct((seqs, width), low),
            jax.ShapeDtypeStruct((share, BLOCKS, heads), wide),
            jax.ShapeDtypeStruct((BLOCKS, share, head_dim), wide),
            jax.ShapeDtypeStruct((BLOCKS, share, head_dim), wide),
            jax.ShapeDtypeStruct((BLOCKS, share, head_dim), wide),
        ),
        in_specs=[in_vmem] * 5 + [in_hbm] * 8,
        out_specs=[in_vmem] * 5,
        scratch_shapes=[
            per_block((4, head_dim, span), low),
            per_block((2 * heads, span), low),
            per_block((head_dim, span), low),
            per_block((share, head_dim, head_dim), wide),
            per_block((share, head_dim, head_dim), low),
            per_block((n_tp, seqs, width), low),
            pltpu.VMEM((seqs, 4 * head_dim + LANES), wide),
            per_block((n_dp, pad, 4 * head_dim), low),
            per_block((n_dp, pad, 4 * head_dim), low),
            per_block((n_dp, pad, LANES), wide),
            per_block((n_dp, pad, LANES), wide),
            per_block((n_dp, pad, head_dim), low),
            pltpu.VMEM((seqs, head_dim), wide),
            per_block((n_tp, seqs, width), low),
            per_block((n_tp, seqs, width), low),
            sems(7),
            pltpu.SemaphoreType.DMA((BLOCKS,)),
            sems(n_tp),
            sems(n_tp),
            sems(n_dp),
            sems(n_dp),
            sems(n_dp),
            sems(n_dp),
            sems(n_dp),
            sems(n_dp),
            sems(n_tp),
            sems(n_tp),
        ],
        compiler_params=pltpu.CompilerParams(
            collective_id=0, has_side_effects=True
        ),
        cost_estimate=pl.CostEstimate(
            flops=10 * BLOCKS * seqs * head_dim * span,
            bytes_accessed=40 * BLOCKS * head_dim * span,
            transcendentals=0,
        ),
        name="both_blocks",
    )(
        residual_in, norm_gain, forget_bias, head_gain, mem_stab.transpose(1, 0, 2),
        w_query, w_key, w_value, w_outgate, w_igate.swapaxes(1, 2), w_fgate.swapaxes(1, 2),
        w_proj, mem_matrix,
    )
    one_block = lambda *dims: pl.BlockSpec((1,) + dims, lambda j: (j,) + (0,) * len(dims))
    whole = lambda *dims: pl.BlockSpec(dims, lambda j: (0,) * len(dims))
    matrix, out, stab_new = pl.pallas_call(
        update_kernel,
        grid=(BLOCKS,),
        out_shape=(
            jax.ShapeDtypeStruct(mem_matrix.shape, wide),
            jax.ShapeDtypeStruct(out.shape, low),
            jax.ShapeDtypeStruct(stab_new.shape, wide),
        ),
        in_specs=[one_block(share, head_dim)] * 3
        + [one_block(share, head_dim, head_dim), whole(*out.shape), whole(*stab_new.shape)],
        out_specs=(
            one_block(share, head_dim, head_dim), whole(*out.shape), whole(*stab_new.shape)
        ),
        scratch_shapes=[pltpu.VMEM((pad, head_dim), wide)],
        name="memory_update",
    )(keep, value, key, mem_matrix, out, stab_new)
    return out, matrix, stab_new.transpose(1, 0, 2)


def solution(mesh):
    in_specs = (
        P(None, ("dp", "tp")),
        P(None, "dp"),
        P(None, "tp", "dp"),
        P(None, "tp", "dp"),
        P(None, "tp", "dp"),
        P(None, "tp", "dp"),
        P(),
        P(),
        P(),
        P(None, "tp"),
        P(None, "tp", "dp"),
        P(None, "dp", "tp", None),
        P(None, "dp", None),
    )
    out_specs = (P(None, ("dp", "tp")), P(None, "dp", "tp", None), P(None, "dp", None))
    n_tp, n_dp = mesh.shape["tp"], mesh.shape["dp"]

    def fits(residual_in, w_query, w_igate):
        width = residual_in.shape[1] // (n_tp * n_dp)
        return (
            w_query.shape[1] == n_tp * HEAD_DIM
            and width % LANES == 0
            and n_tp > 1
            and n_tp & (n_tp - 1) == 0
            and w_igate.shape[2] % 16 == 0
            and residual_in.shape[0] % n_dp == 0
        )

    def run(residual_in, norm_gain, w_query, *others):
        if fits(residual_in, w_query, others[3]):
            body = functools.partial(fused_device, n_tp, n_dp)
        else:
            body = per_device
        step = jax.shard_map(
            body, mesh=mesh, in_specs=in_specs, out_specs=out_specs, check_vma=False
        )
        return step(residual_in, norm_gain, w_query, *others)

    return run
```
